256 devices in a mesh: grp: 2 (over y), sp: 32 (over z, core), tp: 4 (over x).
Axes of the slice: x: 4, y: 2, z: 16, core: 2. Of those that a mesh axis runs over, the one named last changes fastest.
The devices are a block of a 4x16x16 slice.
Arguments:
- queries: bfloat16 [16384, 2048], P(('grp', 'sp'), 'tp'), parts along dimension 0, may hold values from -6 to 6
- keys: bfloat16 [16384, 512], P(('grp', 'sp'), 'tp'), parts along dimension 0, may hold values from -6 to 6
- values: bfloat16 [16384, 512], P(('grp', 'sp'), 'tp'), parts along dimension 0, may hold values from -6 to 6
- query_gain: float32 [128], replicated, may hold values from 1 to 5, as said below
- key_norm_gain: float32 [128], replicated, may hold values from 1 to 5, as said below
- out_weight: bfloat16 [2048, 2048], P('tp'), may hold values from -0.125 to 0.125
- residual: bfloat16 [16384, 2048], P(('grp', 'sp')), parts along dimension 0, may hold values from -0.59765625 to 0.59765625
- mixer_gain: float32 [2048], replicated, may hold values from 0.1 to 1.9
- gate_weight: bfloat16 [2048, 5632], P('sp', 'tp'), may hold values from -0.125 to 0.125
- up_weight: bfloat16 [2048, 5632], P('sp', 'tp'), may hold values from -0.125 to 0.125
- conv_taps: float32 [3, 5632], P(None, 'tp'), may hold values from -3.5 to 3.5
- down_weight: bfloat16 [5632, 2048], P('tp', 'sp'), may hold values from -0.078125 to 0.078125
Outputs:
- layer_out: bfloat16 [16384, 2048], P(('grp', 'sp', 'tp')), parts along dimension 0
The draws below stay inside these ranges and needn't reach their ends.
There are 2 independent parts, one for each index of `grp`. The reference program is written for one: setup_inputs(seed, part) draws one part's arguments, and reference() takes and returns one part's arrays. A program takes and returns all parts, laid end to end along the dimension named above; an argument that names none is the same for every part. Nothing has to cross between parts.
Inputs may be any that keep to these rules, and one draw needn't show every extreme that they name: `query_gain`: positive. `key_norm_gain`: positive.
All inputs are finite; a program needn't handle non-finite values.
Results may differ from the reference program's by a relative error of at most 0.024.
Values may be sent and summed in bfloat16 or wider, within the bound.
No kernel may reach another device: no remote copies, remote signals or barrier semaphores. Data moves between devices by JAX's collectives and lax.ppermute only.
A program may use at most 128 MiB of HBM per device.

```python
import math
import jax
import jax.numpy as jnp
from jax import lax

D = 2048
FF = 5632
QUERY_HEADS = 16
KEY_VALUE_HEADS = 4
HEAD_SIZE = 128
GRID = 64
SEQUENCE_TOKENS = 8192


def grouped_keys(key):
    unit_keys = jax.random.normal(jax.random.fold_in(key, 11), (SEQUENCE_TOKENS, KEY_VALUE_HEADS * HEAD_SIZE), jnp.float32)
    return jnp.clip(unit_keys, -6.0, 6.0)


def draw_keys(key, part):
    return grouped_keys(key).astype(jnp.bfloat16)


def draw_queries(key, part):
    drawn = jnp.clip(jax.random.normal(jax.random.fold_in(key, 12), (SEQUENCE_TOKENS, QUERY_HEADS * HEAD_SIZE), jnp.float32), -6.0, 6.0)
    return drawn.astype(jnp.bfloat16)


def draw_query_gain(key, part):
    return jax.random.uniform(jax.random.fold_in(key, 21), (HEAD_SIZE,), jnp.float32, 1.0, 1.8)


def draw_key_norm_gain(key, part):
    return jax.random.uniform(jax.random.fold_in(key, 22), (HEAD_SIZE,), jnp.float32, 1.0, 1.8)


def block_levels(key, dims, shards, low, top_value):
    loudness, own = 1.0, jax.random.fold_in(key, 6)
    for axis_at, blocks in shards:
        draws = jnp.exp(jax.random.uniform(jax.random.fold_in(own, axis_at), (blocks,), jnp.float32, low / len(shards), top_value / len(shards)))
        loudness = loudness * jnp.repeat(draws, dims[axis_at] // blocks).reshape([-1 if axis == axis_at else 1 for axis in range(len(dims))])
    return loudness


def centred(key, dims, deviation, bound, pieces=(), kind=jnp.bfloat16):
    level = block_levels(key, dims, pieces, -0.22, 0.18) if pieces else 1.0
    values = jax.random.normal(key, dims, jnp.float32) * deviation * level
    return jnp.minimum(jnp.maximum(values, -bound), bound).astype(kind)


def setup_inputs(seed: int = 0, part: int = 0) -> dict:
    seeds = jax.random.split(jax.random.key(seed), 13)
    part_splits = jax.random.split(jax.random.fold_in(seeds[12], part), 13)
    return {
        "queries": draw_queries(jax.random.fold_in(jax.random.fold_in(seeds[12], part), 71), part),
        "keys": draw_keys(jax.random.fold_in(jax.random.fold_in(seeds[12], part), 71), part),
        "values": centred(part_splits[2], (SEQUENCE_TOKENS, KEY_VALUE_HEADS * HEAD_SIZE), 1.0, 6.0, ((0, 32), (1, 4))),
        "query_gain": draw_query_gain(jax.random.fold_in(seeds[12], 71), part),
        "key_norm_gain": draw_key_norm_gain(jax.random.fold_in(seeds[12], 71), part),
        "out_weight": centred(seeds[5], (QUERY_HEADS * HEAD_SIZE, D), (QUERY_HEADS * HEAD_SIZE) ** -0.5, 0.125, ((0, 4),)),
        "residual": centred(part_splits[6], (SEQUENCE_TOKENS, D), 0.1, 0.59765625, ((0, 32),)),
        "mixer_gain": jnp.clip(1.0 + 0.18 * jax.random.normal(seeds[7], (D,), jnp.float32), 0.1, 1.9),
        "gate_weight": centred(seeds[8], (D, FF), D ** -0.5, 0.125, ((0, 32), (1, 4))),
        "up_weight": centred(seeds[9], (D, FF), D ** -0.5, 0.125, ((0, 32), (1, 4))),
        "conv_taps": centred(seeds[10], (3, FF), 3 ** -0.5, 3.5, ((1, 4),), jnp.float32),
        "down_weight": centred(seeds[11], (FF, D), FF ** -0.5, 0.078125, ((0, 4), (1, 32))),
    }


norm_eps = 1e-06
rope_base = 10000.0

def angle_tables(positions, head_dim):
    quarter = head_dim // 4
    freqs = 1.0 / rope_base ** (jnp.arange(quarter, dtype=jnp.float32) * 4.0 / head_dim)
    grid_row = (positions // GRID).astype(jnp.float32)
    grid_col = (positions % GRID).astype(jnp.float32)
    by_row = grid_row[:, None] * freqs[None, :]
    by_col = grid_col[:, None] * freqs[None, :]
    angles = jnp.concatenate([by_row, by_row, by_col, by_col], axis=-1)
    return (jnp.cos(angles), jnp.sin(angles))

def apply_rotary(field, cosine_table, sine_table):
    half = field.shape[-1] // 2
    quarter = half // 2
    first = field[..., :half]
    second = field[..., half:]
    turned = jnp.concatenate([-first[..., quarter:], first[..., :quarter], -second[..., quarter:], second[..., :quarter]], axis=-1)
    return field * cosine_table[:, None, :] + turned * sine_table[:, None, :]

def per_head_norm(field, gain):
    floats = field.astype(jnp.float32)
    return floats * lax.rsqrt(lax.optimization_barrier(jnp.mean(floats * floats, axis=-1, keepdims=True)) + norm_eps) * gain

def reference(queries, keys, values, query_gain, key_norm_gain, out_weight, residual, mixer_gain, gate_weight, up_weight, conv_taps, down_weight):
    query_group = QUERY_HEADS // KEY_VALUE_HEADS
    positions = jnp.arange(SEQUENCE_TOKENS, dtype=jnp.int32)
    cosine_table, sine_table = angle_tables(positions, HEAD_SIZE)
    rotated_queries = apply_rotary(per_head_norm(queries.reshape(SEQUENCE_TOKENS, QUERY_HEADS, HEAD_SIZE), query_gain), cosine_table, sine_table).astype(jnp.bfloat16)
    rotated_keys = apply_rotary(per_head_norm(keys.reshape(SEQUENCE_TOKENS, KEY_VALUE_HEADS, HEAD_SIZE), key_norm_gain), cosine_table, sine_table).astype(jnp.bfloat16)
    key_all = rotated_keys.astype(jnp.float32)
    value_rows_full = values.reshape(SEQUENCE_TOKENS, KEY_VALUE_HEADS, HEAD_SIZE).astype(jnp.float32)
    block_slice = math.gcd(SEQUENCE_TOKENS, 512)
    query_block_list = rotated_queries.reshape(SEQUENCE_TOKENS // block_slice, block_slice, KEY_VALUE_HEADS, query_group, HEAD_SIZE)
    scale = HEAD_SIZE ** (-0.5)

    def one_block(query_block):
        scores = jnp.einsum('qhgd,khd->hgqk', query_block.astype(jnp.float32), key_all) * scale
        expo = jnp.exp(scores - lax.optimization_barrier(jnp.max(scores, axis=-1, keepdims=True)))
        totals = lax.optimization_barrier(jnp.sum(expo, axis=-1))
        weights = lax.optimization_barrier(expo.astype(jnp.bfloat16)).astype(jnp.float32)
        summed = jnp.einsum('hgqk,khd->qhgd', weights, value_rows_full)
        return (summed / jnp.transpose(totals, (2, 0, 1))[..., None]).astype(jnp.bfloat16)
    heads = lax.map(one_block, query_block_list).reshape(SEQUENCE_TOKENS, QUERY_HEADS * HEAD_SIZE)
    mixed = residual.astype(jnp.float32) + jnp.dot(heads, out_weight, preferred_element_type=jnp.float32)
    normed = per_head_norm(mixed, mixer_gain).astype(jnp.bfloat16)
    gate = jnp.dot(normed, gate_weight, preferred_element_type=jnp.float32).astype(jnp.bfloat16)
    up_val = jnp.dot(normed, up_weight, preferred_element_type=jnp.float32).astype(jnp.bfloat16)
    padded = jnp.pad(gate.astype(jnp.float32), ((1, 1), (0, 0)))
    conv = conv_taps[0] * padded[:-2] + conv_taps[1] * padded[1:-1] + conv_taps[2] * padded[2:]
    hidden = (jax.nn.silu(conv) * up_val.astype(jnp.float32)).astype(jnp.bfloat16)
    layer_out = mixed + jnp.dot(hidden, down_weight, preferred_element_type=jnp.float32)
    return layer_out.astype(jnp.bfloat16)
```

```python
import math

import numpy as np
import jax
import jax.numpy as jnp
from jax import lax
from jax.experimental import pallas as pl
from jax.experimental.pallas import tpu as pltpu
from jax.sharding import PartitionSpec as P

GRID = 64
NORM_EPS = 1e-06
ROPE_BASE = 10000.0


def split_up(array, dim, peers):
    before, after = (array.shape[:dim], array.shape[dim + 1 :])
    return jnp.moveaxis(array.reshape(*before, peers, -1, *after), dim, 0)


def sum_at_owner(array, axis, dim):
    parts = split_up(array, dim, lax.axis_size(axis))
    arrived = lax.all_to_all(parts, axis, split_axis=0, concat_axis=0, tiled=True)
    return arrived.astype(jnp.float32).sum(axis=0)


def collect(array, axis):
    copies = jnp.broadcast_to(array, (lax.axis_size(axis), *array.shape))
    parts = lax.all_to_all(copies, axis, split_axis=0, concat_axis=0, tiled=True)
    return parts.reshape(-1, array.shape[-1])


def row_norm(field, gain):
    return field * lax.rsqrt(jnp.mean(field * field, axis=-1, keepdims=True) + NORM_EPS) * gain


def rope_kernel(base, q_in, k_in, v_in, q_gain, k_gain, freqs, q_out, kv_out, *, q_scale):
    rows, head = k_in.shape[0], q_gain.shape[-1]
    quarter = head // 4
    lane = lax.broadcasted_iota(jnp.int32, (rows, head), 1)
    position = base[0] + lax.broadcasted_iota(jnp.int32, (rows, head), 0)
    bits = GRID.bit_length() - 1
    place = jnp.where(lane < head // 2, jnp.right_shift(position, bits), position & (GRID - 1))
    angle = place.astype(jnp.float32) * freqs[...]
    cosine, sine = jnp.cos(angle), jnp.sin(angle)
    first = (lane & (2 * quarter - 1)) < quarter

    def rotated(x, gain):
        y = row_norm(x.astype(jnp.float32), gain)
        turned = jnp.where(first, -pltpu.roll(y, head - quarter, 1), pltpu.roll(y, quarter, 1))
        return y * cosine + turned * sine

    for h in range(q_in.shape[1] // head):
        at = slice(h * head, (h + 1) * head)
        q_out[:, at] = (rotated(q_in[:, at], q_gain[...]) * q_scale).astype(q_out.dtype)
    kv_out[:, :head] = rotated(k_in[...], k_gain[...]).astype(kv_out.dtype)
    kv_out[:, head:] = v_in[...]


def rope(base, queries, keys, values, query_gain, key_gain):
    rows, head = keys.shape
    quarter = head // 4
    by_axis = 1.0 / ROPE_BASE ** (np.arange(quarter, dtype=np.float64) * 4.0 / head)
    freqs = jnp.asarray(np.tile(by_axis, 4)[None].astype(np.float32))
    scale = head**-0.5 * math.log2(math.e)
    vmem = pl.BlockSpec(memory_space=pltpu.VMEM)
    return pl.pallas_call(
        lambda *refs: rope_kernel(*refs, q_scale=scale),
        out_shape=(
            jax.ShapeDtypeStruct(queries.shape, jnp.bfloat16),
            jax.ShapeDtypeStruct((rows, 2 * head), jnp.bfloat16),
        ),
        in_specs=[pl.BlockSpec(memory_space=pltpu.SMEM)] + [vmem] * 6,
        out_specs=(vmem, vmem),
        compiler_params=pltpu.CompilerParams(vmem_limit_bytes=16 << 20),
        name="rope",
    )(base, queries, keys, values, query_gain[None], key_gain[None], freqs)


def attend_kernel(*refs, count, first, last, half):
    own_q, pair_q = refs[:2]
    chunks = refs[2 : 2 + count]
    rest = refs[2 + count :]
    head = own_q.shape[-1]
    step = pl.program_id(0)
    q = jnp.where(step < half, own_q[...], pair_q[...])
    scores = [
        lax.dot_general(
            q, c[:, :head], (((1,), (1,)), ((), ())), preferred_element_type=jnp.float32
        )
        for c in chunks
    ]
    tops = scores[0]
    for s in scores[1:]:
        tops = jnp.maximum(tops, s)
    top = jnp.max(tops, axis=-1, keepdims=True)
    if not first:
        acc_in, top_in, sum_in = rest[:3]
        rest = rest[3:]
        before = top_in[:, :1]
        top = jnp.maximum(top, before)
        factor = jnp.exp2(before - top)
    partial, summed = None, None
    for s, c in zip(scores, chunks):
        expo = jnp.exp2(s - top)
        here = sum(expo[:, i : i + head] for i in range(0, expo.shape[1], head))
        summed = here if summed is None else summed + here
        product = jnp.dot(
            expo.astype(jnp.bfloat16), c[:, head:], preferred_element_type=jnp.float32
        )
        partial = product if partial is None else partial + product
    if not first:
        partial = partial + acc_in[...] * factor
        summed = summed + sum_in[...] * factor
    if not last:
        acc_out, top_out, sum_out = rest
        acc_out[...] = partial
        top_out[...] = jnp.broadcast_to(top, top_out.shape)
        sum_out[...] = summed
        return
    own_out, pair_out = rest
    total = jnp.sum(summed, axis=-1, keepdims=True)
    mean = partial / total
    level = jnp.broadcast_to(top + jnp.log2(total), mean.shape)

    @pl.when(step < half)
    def _():
        own_out[:, :head] = mean
        own_out[:, head:] = level

    @pl.when(step >= half)
    def _():
        pair_out[:, :head] = mean
        pair_out[:, head:] = level


def attend(own_q, pair_q, chunks, state, last):
    rows, width = own_q.shape
    head = chunks[0].shape[1] // 2
    half = width // head
    steps = 2 * half
    first = state is None
    q_specs = [
        pl.BlockSpec((rows, head), lambda g: (0, jnp.minimum(g, half - 1))),
        pl.BlockSpec((rows, head), lambda g: (0, jnp.maximum(g - half, 0))),
    ]
    kv_specs = [pl.BlockSpec(c.shape, lambda g: (0, 0)) for c in chunks]
    block = pl.BlockSpec((rows, head), lambda g: (g, 0))
    whole = jax.ShapeDtypeStruct((steps * rows, head), jnp.float32)
    operands = [own_q, pair_q, *chunks] + ([] if first else list(state))
    in_specs = q_specs + kv_specs + ([] if first else [block] * 3)
    if last:
        out_shape = (jax.ShapeDtypeStruct((half * rows, 2 * head), jnp.float32),) * 2
        out_specs = (
            pl.BlockSpec((rows, 2 * head), lambda g: (jnp.minimum(g, half - 1), 0)),
            pl.BlockSpec((rows, 2 * head), lambda g: (jnp.maximum(g - half, 0), 0)),
        )
    else:
        out_shape, out_specs = ((whole,) * 3, (block,) * 3)
    keys = sum(c.shape[0] for c in chunks)
    return pl.pallas_call(
        lambda *refs: attend_kernel(*refs, count=len(chunks), first=first, last=last, half=half),
        grid=(steps,),
        out_shape=out_shape,
        in_specs=in_specs,
        out_specs=out_specs,
        compiler_params=pltpu.CompilerParams(
            dimension_semantics=("arbitrary",), vmem_limit_bytes=24 << 20
        ),
        cost_estimate=pl.CostEstimate(
            flops=16 * steps * rows * keys * head,
            bytes_accessed=steps * rows * head * 24,
            transcendentals=steps * rows * keys,
        ),
        name="attend",
    )(*operands)


def merge_kernel(own, other, heads):
    rows = heads.shape[0]
    head = own.shape[1] // 2
    for h in range(heads.shape[1] // head):
        at = slice(h * rows, (h + 1) * rows)
        a, b = own[at, head:], other[at, head:]
        top = jnp.maximum(a, b)
        wa, wb = jnp.exp2(a - top), jnp.exp2(b - top)
        mixed = (own[at, :head] * wa + other[at, :head] * wb) / (wa + wb)
        heads[:, h * head : (h + 1) * head] = mixed.astype(heads.dtype)


def merge(own, other, rows, width):
    vmem = pl.BlockSpec(memory_space=pltpu.VMEM)
    return pl.pallas_call(
        merge_kernel,
        out_shape=jax.ShapeDtypeStruct((rows, width), jnp.bfloat16),
        in_specs=[vmem, vmem],
        out_specs=vmem,
        compiler_params=pltpu.CompilerParams(vmem_limit_bytes=16 << 20),
        name="merge",
    )(own, other)


def ffn_kernel(x, taps, weights, out, w_vmem, hidden, sems, *, spans, rows, units):
    copies = []
    for which in range(2):
        for i, (lo, size) in enumerate(spans):
            at = pl.ds(which * units + lo, size)
            copies.append(
                pltpu.make_async_copy(
                    weights.at[:, at], w_vmem.at[:, at], sems.at[which, i]
                )
            )
    tail = pl.ds(2 * units, units)
    outs = out.shape[1]
    block = math.gcd(outs, 512)
    downs = [
        pltpu.make_async_copy(
            weights.at[pl.ds(d, block), tail], w_vmem.at[pl.ds(d, block), tail], sems.at[2, j]
        )
        for j, d in enumerate(range(0, outs, block))
    ]
    n = len(spans)
    for i in range(n):
        copies[i].start()
        copies[n + i].start()
    for c in downs:
        c.start()
    edge = lax.broadcasted_iota(jnp.int32, (rows, 1), 0)
    for i, (lo, size) in enumerate(spans):
        at = slice(lo, lo + size)
        copies[i].wait()
        gate_all = jnp.dot(x[...], w_vmem[:, at], preferred_element_type=jnp.float32)
        gate_all = gate_all.astype(jnp.bfloat16).astype(jnp.float32)
        gate = gate_all[:rows]
        low = jnp.where(edge == 0, gate_all[rows : rows + 1], pltpu.roll(gate, 1, 0))
        high = jnp.where(
            edge == rows - 1, gate_all[rows + 1 : rows + 2], pltpu.roll(gate, rows - 1, 0)
        )
        conv = taps[0:1, at] * low + taps[1:2, at] * gate + taps[2:3, at] * high
        copies[n + i].wait()
        up = jnp.dot(
            x[:rows], w_vmem[:, units + lo : units + lo + size], preferred_element_type=jnp.float32
        )
        up = up.astype(jnp.bfloat16).astype(jnp.float32)
        hidden[:, at] = (conv / (1.0 + jnp.exp(-conv)) * up).astype(hidden.dtype)
    for j, d in enumerate(range(0, outs, block)):
        downs[j].wait()
        out[:, d : d + block] = lax.dot_general(
            hidden[...],
            w_vmem[d : d + block, 2 * units :],
            (((1,), (1,)), ((), ())),
            preferred_element_type=jnp.float32,
        ).astype(out.dtype)


def ffn(x, taps, weights, rows):
    units = taps.shape[1]
    width = weights.shape[0]
    spans = [(lo, min(256, units - lo)) for lo in range(0, units, 256)]
    blocks = width // math.gcd(width, 512)
    vmem = pl.BlockSpec(memory_space=pltpu.VMEM)
    return pl.pallas_call(
        lambda *refs: ffn_kernel(*refs, spans=spans, rows=rows, units=units),
        out_shape=jax.ShapeDtypeStruct((rows, width), jnp.bfloat16),
        in_specs=[vmem, vmem, pl.BlockSpec(memory_space=pl.ANY)],
        out_specs=vmem,
        scratch_shapes=[
            pltpu.VMEM(weights.shape, jnp.bfloat16),
            pltpu.VMEM((rows, units), jnp.bfloat16),
            pltpu.SemaphoreType.DMA((3, max(len(spans), blocks))),
        ],
        compiler_params=pltpu.CompilerParams(vmem_limit_bytes=40 << 20),
        cost_estimate=pl.CostEstimate(
            flops=6 * rows * units * width,
            bytes_accessed=2 * weights.size,
            transcendentals=rows * units,
        ),
        name="ffn",
    )(x, taps, weights)


def local(
    queries,
    keys,
    values,
    query_gain,
    key_norm_gain,
    out_weight,
    residual,
    mixer_gain,
    gate_weight,
    up_weight,
    conv_taps,
    down_weight,
):
    rows, width = queries.shape
    part_rows = rows // lax.axis_size("tp")
    shards = lax.axis_size("sp")
    ring = shards // 2
    weights = lax.all_gather(
        jnp.concatenate([gate_weight, up_weight, down_weight.T], axis=1), "sp", axis=0, tiled=True
    )
    base = (lax.axis_index("sp") * rows).astype(jnp.int32).reshape(1)
    own_q, own_kv = rope(base, queries, keys, values, query_gain, key_norm_gain)

    pair = [(s, s ^ 1) for s in range(shards)]
    ahead = [(s, (s + 2) % shards) for s in range(shards)]
    behind = [(t, s) for s, t in ahead]
    pair_q = lax.ppermute(own_q, "sp", pair)
    up, down = own_kv, own_kv
    ready, state = [own_kv], None
    for hop in range(1, ring // 2 + 1):
        up = lax.ppermute(up, "sp", ahead)
        ready.append(up)
        if 2 * hop < ring:
            down = lax.ppermute(down, "sp", behind)
            ready.append(down)
        end = 2 * hop >= ring
        if end or hop % 2 == 0:
            state = attend(own_q, pair_q, ready, state, end)
            ready = []
    own_part, pair_part = state
    heads = merge(own_part, lax.ppermute(pair_part, "sp", pair), rows, width)

    own_start = lax.axis_index("tp") * part_rows
    projected = sum_at_owner(
        jnp.dot(heads, out_weight, preferred_element_type=jnp.float32).astype(jnp.bfloat16), "tp", 0
    )
    own_resid = lax.dynamic_slice_in_dim(residual, own_start, part_rows, 0)
    mixed = own_resid.astype(jnp.float32) + projected
    normed = collect(row_norm(mixed, mixer_gain).astype(jnp.bfloat16), "tp")
    onward = [(s, s + 1) for s in range(shards - 1)]
    backward = [(t, s) for s, t in onward]
    before = lax.ppermute(normed[-1:], "sp", onward)
    after = lax.ppermute(normed[:1], "sp", backward)
    spare = jnp.zeros((14, normed.shape[1]), normed.dtype)
    extended = jnp.concatenate([normed, before, after, spare], axis=0)
    partial = ffn(extended, conv_taps, weights, rows)
    return (mixed + sum_at_owner(partial, "tp", 0)).astype(jnp.bfloat16)


def solution(mesh):
    in_specs = (
        P(("grp", "sp"), "tp"),
        P(("grp", "sp"), "tp"),
        P(("grp", "sp"), "tp"),
        P(),
        P(),
        P("tp", None),
        P(("grp", "sp"), None),
        P(),
        P("sp", "tp"),
        P("sp", "tp"),
        P(None, "tp"),
        P("tp", "sp"),
    )
    out_specs = P(("grp", "sp", "tp"), None)
    return jax.shard_map(local, mesh=mesh, in_specs=in_specs, out_specs=out_specs, check_vma=False)
```

```python
import math

import numpy as np
import jax
import jax.numpy as jnp
from jax import lax
from jax.experimental import pallas as pl
from jax.experimental.pallas import tpu as pltpu
from jax.sharding import PartitionSpec as P

GRID = 64
NORM_EPS = 1e-06
ROPE_BASE = 10000.0


def split_up(array, dim, peers):
    before, after = (array.shape[:dim], array.shape[dim + 1 :])
    return jnp.moveaxis(array.reshape(*before, peers, -1, *after), dim, 0)


def sum_at_owner(array, axis, dim):
    parts = split_up(array, dim, lax.axis_size(axis))
    arrived = lax.all_to_all(parts, axis, split_axis=0, concat_axis=0, tiled=True)
    return arrived.astype(jnp.float32).sum(axis=0)


def collect(array, axis):
    copies = jnp.broadcast_to(array, (lax.axis_size(axis), *array.shape))
    parts = lax.all_to_all(copies, axis, split_axis=0, concat_axis=0, tiled=True)
    return parts.reshape(-1, array.shape[-1])


def row_norm(field, gain):
    return field * lax.rsqrt(jnp.mean(field * field, axis=-1, keepdims=True) + NORM_EPS) * gain


def rope_kernel(base, *refs, q_scale):
    q_out, kv_out = refs[6:8]
    q_in, k_in, v_in, q_gain, k_gain, freqs = refs[8:14]
    sems = refs[14]
    copies = [
        pltpu.make_async_copy(refs[i], refs[8 + i], sems.at[i]) for i in (5, 4, 1, 2, 3, 0)
    ]
    for c in copies:
        c.start()
    rows, head = k_in.shape
    quarter = head // 4
    lane = lax.broadcasted_iota(jnp.int32, (rows, head), 1)
    position = base[0] + lax.broadcasted_iota(jnp.int32, (rows, head), 0)
    bits = GRID.bit_length() - 1
    place = jnp.where(lane < head // 2, jnp.right_shift(position, bits), position & (GRID - 1))
    for c in copies:
        c.wait()
    angle = place.astype(jnp.float32) * freqs[...]
    cosine, sine = jnp.cos(angle), jnp.sin(angle)
    first = (lane & (2 * quarter - 1)) < quarter

    def rotated(x, gain):
        y = row_norm(x.astype(jnp.float32), gain)
        turned = jnp.where(first, -pltpu.roll(y, head - quarter, 1), pltpu.roll(y, quarter, 1))
        return y * cosine + turned * sine

    kv_out[:, :head] = rotated(k_in[...], k_gain[...]).astype(kv_out.dtype)
    kv_out[:, head:] = v_in[...]
    for h in range(q_in.shape[1] // head):
        at = slice(h * head, (h + 1) * head)
        q_out[:, at] = (rotated(q_in[:, at], q_gain[...]) * q_scale).astype(q_out.dtype)


def rope(base, queries, keys, values, query_gain, key_gain):
    rows, head = keys.shape
    quarter = head // 4
    by_axis = 1.0 / ROPE_BASE ** (np.arange(quarter, dtype=np.float64) * 4.0 / head)
    freqs = jnp.asarray(np.tile(by_axis, 4)[None].astype(np.float32))
    scale = head**-0.5 * math.log2(math.e)
    vmem = pl.BlockSpec(memory_space=pltpu.VMEM)
    operands = (queries, keys, values, query_gain[None], key_gain[None], freqs)
    return pl.pallas_call(
        lambda *refs: rope_kernel(*refs, q_scale=scale),
        out_shape=(
            jax.ShapeDtypeStruct(queries.shape, jnp.bfloat16),
            jax.ShapeDtypeStruct((rows, 2 * head), jnp.bfloat16),
        ),
        in_specs=[pl.BlockSpec(memory_space=pltpu.SMEM)]
        + [pl.BlockSpec(memory_space=pltpu.HBM)] * len(operands),
        out_specs=(vmem, vmem),
        scratch_shapes=[pltpu.VMEM(x.shape, x.dtype) for x in operands]
        + [pltpu.SemaphoreType.DMA((len(operands),))],
        compiler_params=pltpu.CompilerParams(vmem_limit_bytes=16 << 20),
        name="rope",
    )(base, *(pltpu.with_memory_space_constraint(x, pltpu.HBM) for x in operands))


def attend_kernel(*refs, count, first, last):
    own_q, pair_q = refs[:2]
    chunks = refs[2 : 2 + count]
    rest = refs[2 + count :]
    rows = own_q.shape[0]
    head = chunks[0].shape[1] // 2
    if not first:
        acc_in, top_in, sum_in = rest[:3]
        rest = rest[3:]

    def one(h, carry):
        lanes = pl.ds(pl.multiple_of(h * head, head), head)
        at = [pl.ds(pl.multiple_of((2 * h + i) * rows, rows), rows) for i in range(2)]
        scores = [
            [
                lax.dot_general(
                    q[:, lanes],
                    c[:, :head],
                    (((1,), (1,)), ((), ())),
                    preferred_element_type=jnp.float32,
                )
                for c in chunks
            ]
            for q in (own_q, pair_q)
        ]
        for i in range(2):
            tops = None
            for s in scores[i]:
                for j in range(0, s.shape[1], head):
                    piece = s[:, j : j + head]
                    tops = piece if tops is None else jnp.maximum(tops, piece)
            top = jnp.max(tops, axis=-1, keepdims=True)
            if not first:
                before = top_in[at[i], :1]
                top = jnp.maximum(top, before)
                factor = jnp.exp2(before - top)
            partial, summed = None, None
            for s, c in zip(scores[i], chunks):
                expo = jnp.exp2(s - top)
                for j in range(0, expo.shape[1], head):
                    piece = expo[:, j : j + head]
                    summed = piece if summed is None else summed + piece
                product = jnp.dot(
                    expo.astype(jnp.bfloat16), c[:, head:], preferred_element_type=jnp.float32
                )
                partial = product if partial is None else partial + product
            if not first:
                partial = partial + acc_in[at[i]] * factor
                summed = summed + sum_in[at[i]] * factor
            if not last:
                acc_out, top_out, sum_out = rest
                acc_out[at[i]] = partial
                top_out[at[i]] = jnp.broadcast_to(top, partial.shape)
                sum_out[at[i]] = summed
            else:
                total = jnp.sum(summed, axis=-1, keepdims=True)
                out = rest[i]
                to = pl.ds(pl.multiple_of(h * rows, rows), rows)
                out[to, :head] = partial / total
                out[to, head:] = jnp.broadcast_to(top + jnp.log2(total), partial.shape)
        return carry

    lax.fori_loop(0, own_q.shape[1] // head, one, 0)


def attend(own_q, pair_q, chunks, state, last):
    rows, width = own_q.shape
    head = chunks[0].shape[1] // 2
    half = width // head
    first = state is None
    vmem = pl.BlockSpec(memory_space=pltpu.VMEM)
    operands = [own_q, pair_q, *chunks] + ([] if first else list(state))
    shapes = [(half * rows, 2 * head)] * 2 if last else [(2 * half * rows, head)] * 3
    begin = 2 + len(chunks)
    aliases = {} if first or last else {begin + i: i for i in range(3)}
    keys = sum(c.shape[0] for c in chunks)
    return pl.pallas_call(
        lambda *refs: attend_kernel(*refs, count=len(chunks), first=first, last=last),
        out_shape=tuple(jax.ShapeDtypeStruct(s, jnp.float32) for s in shapes),
        in_specs=[vmem] * len(operands),
        out_specs=(vmem,) * len(shapes),
        input_output_aliases=aliases,
        compiler_params=pltpu.CompilerParams(vmem_limit_bytes=16 << 20),
        cost_estimate=pl.CostEstimate(
            flops=8 * half * rows * keys * head,
            bytes_accessed=2 * half * rows * head * 24,
            transcendentals=2 * half * rows * keys,
        ),
        name="attend",
    )(*operands)


def merge_kernel(own, other, heads):
    rows = heads.shape[0]
    head = own.shape[1] // 2
    for h in range(heads.shape[1] // head):
        at = slice(h * rows, (h + 1) * rows)
        a, b = own[at, head:], other[at, head:]
        top = jnp.maximum(a, b)
        wa, wb = jnp.exp2(a - top), jnp.exp2(b - top)
        mixed = (own[at, :head] * wa + other[at, :head] * wb) / (wa + wb)
        heads[:, h * head : (h + 1) * head] = mixed.astype(heads.dtype)


def merge(own, other, rows, width):
    vmem = pl.BlockSpec(memory_space=pltpu.VMEM)
    return pl.pallas_call(
        merge_kernel,
        out_shape=jax.ShapeDtypeStruct((rows, width), jnp.bfloat16),
        in_specs=[vmem, vmem],
        out_specs=vmem,
        compiler_params=pltpu.CompilerParams(vmem_limit_bytes=16 << 20),
        name="merge",
    )(own, other)


def ffn_kernel(x, taps, weights, out, w_vmem, hidden, sems, *, rows, units, chunk):
    outs = out.shape[1]
    block = math.gcd(outs, 512)
    full, rest = divmod(units, chunk)
    spans = full + (rest > 0)

    def columns(which, i, size):
        at = pl.ds(pl.multiple_of(which * units + i * chunk, 128), size)
        return pltpu.make_async_copy(weights.at[:, at], w_vmem.at[:, at], sems.at[which, i])

    def down(j):
        at = (pl.ds(j * block, block), pl.ds(2 * units, units))
        return pltpu.make_async_copy(weights.at[at], w_vmem.at[at], sems.at[2, j])

    def start(i):
        @pl.when(i < full)
        def _():
            columns(0, i, chunk).start()
            columns(1, i, chunk).start()

        if rest:

            @pl.when(i == full)
            def _():
                columns(0, full, rest).start()
                columns(1, full, rest).start()

        for j in range(outs // block):

            @pl.when(i == spans + j)
            def _():
                down(j).start()

    edge = lax.broadcasted_iota(jnp.int32, (rows, 1), 0)

    def one(i, size):
        at = pl.ds(pl.multiple_of(i * chunk, 128), size)
        up_at = pl.ds(pl.multiple_of(units + i * chunk, 128), size)
        columns(0, i, size).wait()
        gate_all = jnp.dot(x[...], w_vmem[:, at], preferred_element_type=jnp.float32)
        gate_all = gate_all.astype(jnp.bfloat16).astype(jnp.float32)
        gate = gate_all[:rows]
        low = jnp.where(edge == 0, gate_all[rows : rows + 1], pltpu.roll(gate, 1, 0))
        high = jnp.where(
            edge == rows - 1, gate_all[rows + 1 : rows + 2], pltpu.roll(gate, rows - 1, 0)
        )
        conv = taps[0:1, at] * low + taps[1:2, at] * gate + taps[2:3, at] * high
        columns(1, i, size).wait()
        up = jnp.dot(x[:rows], w_vmem[:, up_at], preferred_element_type=jnp.float32)
        up = up.astype(jnp.bfloat16).astype(jnp.float32)
        hidden[:, at] = (conv / (1.0 + jnp.exp(-conv)) * up).astype(hidden.dtype)

    ahead = 2
    for i in range(ahead):
        start(jnp.int32(i))

    def body(i, carry):
        start(i + ahead)
        one(i, chunk)
        return carry

    lax.fori_loop(0, full, body, 0)
    for i in range(full + ahead, spans + outs // block):
        start(jnp.int32(i))
    if rest:
        one(full, rest)
    for j in range(outs // block):
        down(j).wait()
        at = slice(j * block, (j + 1) * block)
        out[:, at] = lax.dot_general(
            hidden[...],
            w_vmem[at, 2 * units :],
            (((1,), (1,)), ((), ())),
            preferred_element_type=jnp.float32,
        ).astype(out.dtype)


def ffn(x, taps, weights, rows):
    units = taps.shape[1]
    width = weights.shape[0]
    chunk = 512
    slots = max(-(-units // chunk), width // math.gcd(width, 512))
    vmem = pl.BlockSpec(memory_space=pltpu.VMEM)
    return pl.pallas_call(
        lambda *refs: ffn_kernel(*refs, rows=rows, units=units, chunk=chunk),
        out_shape=jax.ShapeDtypeStruct((rows, width), jnp.bfloat16),
        in_specs=[vmem, vmem, pl.BlockSpec(memory_space=pl.ANY)],
        out_specs=vmem,
        scratch_shapes=[
            pltpu.VMEM(weights.shape, jnp.bfloat16),
            pltpu.VMEM((rows, units), jnp.bfloat16),
            pltpu.SemaphoreType.DMA((3, slots)),
        ],
        compiler_params=pltpu.CompilerParams(vmem_limit_bytes=40 << 20),
        cost_estimate=pl.CostEstimate(
            flops=6 * rows * units * width,
            bytes_accessed=2 * weights.size,
            transcendentals=rows * units,
        ),
        name="ffn",
    )(x, taps, weights)


def local(
    queries,
    keys,
    values,
    query_gain,
    key_norm_gain,
    out_weight,
    residual,
    mixer_gain,
    gate_weight,
    up_weight,
    conv_taps,
    down_weight,
):
    rows, width = queries.shape
    part_rows = rows // lax.axis_size("tp")
    shards = lax.axis_size("sp")
    ring = shards // 2
    weights = lax.all_gather(
        jnp.concatenate([gate_weight, up_weight, down_weight.T], axis=1), "sp", axis=0, tiled=True
    )
    base = (lax.axis_index("sp") * rows).astype(jnp.int32).reshape(1)
    own_q, own_kv = rope(base, queries, keys, values, query_gain, key_norm_gain)

    pair = [(s, s ^ 1) for s in range(shards)]
    ahead = [(s, (s + 2) % shards) for s in range(shards)]
    behind = [(t, s) for s, t in ahead]
    pair_q = lax.ppermute(own_q, "sp", pair)
    up, down = own_kv, own_kv
    ready, state = [own_kv], None
    hops = ring // 2
    for hop in range(1, hops + 1):
        new_up = lax.ppermute(up, "sp", ahead)
        new_down = lax.ppermute(down, "sp", behind) if 2 * hop < ring else None
        if hop > 1:
            state = attend(own_q, pair_q, ready, state, False)
            ready = []
        up, down = new_up, new_down
        ready += [c for c in (up, down) if c is not None]
        if state is not None and hop < hops:
            up, down, *state = lax.optimization_barrier((up, down, *state))
    own_part, pair_part = attend(own_q, pair_q, ready, state, True)
    heads = merge(own_part, lax.ppermute(pair_part, "sp", pair), rows, width)

    own_start = lax.axis_index("tp") * part_rows
    projected = sum_at_owner(
        jnp.dot(heads, out_weight, preferred_element_type=jnp.float32).astype(jnp.bfloat16), "tp", 0
    )
    own_resid = lax.dynamic_slice_in_dim(residual, own_start, part_rows, 0)
    mixed = own_resid.astype(jnp.float32) + projected
    normed = collect(row_norm(mixed, mixer_gain).astype(jnp.bfloat16), "tp")
    onward = [(s, s + 1) for s in range(shards - 1)]
    backward = [(t, s) for s, t in onward]
    before = lax.ppermute(normed[-1:], "sp", onward)
    after = lax.ppermute(normed[:1], "sp", backward)
    spare = jnp.zeros((14, normed.shape[1]), normed.dtype)
    extended = jnp.concatenate([normed, before, after, spare], axis=0)
    partial = ffn(extended, conv_taps, weights, rows)
    return (mixed + sum_at_owner(partial, "tp", 0)).astype(jnp.bfloat16)


def solution(mesh):
    in_specs = (
        P(("grp", "sp"), "tp"),
        P(("grp", "sp"), "tp"),
        P(("grp", "sp"), "tp"),
        P(),
        P(),
        P("tp", None),
        P(("grp", "sp"), None),
        P(),
        P("sp", "tp"),
        P("sp", "tp"),
        P(None, "tp"),
        P("tp", "sp"),
    )
    out_specs = P(("grp", "sp", "tp"), None)
    return jax.shard_map(local, mesh=mesh, in_specs=in_specs, out_specs=out_specs, check_vma=False)
```
